32 devices in a mesh: grp: 2 (over x), sp: 8 (over z, y), tp: 2 (over core).
Axes of the slice: x: 2, y: 2, z: 4, core: 2. Of those that a mesh axis runs over, the one named last changes fastest.
Arguments:
- resid: bfloat16 [2048, 2048], P(('grp', 'sp')), parts along dimension 0, may hold values from -6 to 6
- queries_first: bfloat16 [2048, 2048], P(('grp', 'sp'), 'tp'), parts along dimension 0, may hold values from -150 to 150
- keys_first: bfloat16 [2048, 2048], P(('grp', 'sp'), 'tp'), parts along dimension 0, may hold values from -6 to 6
- values_first: bfloat16 [2048, 2048], P(('grp', 'sp'), 'tp'), parts along dimension 0, may hold values from -6 to 6
- rel_first: float32 [16, 257], P('tp'), may hold values from -4 to 4
- post_first: float32 [2048], replicated, may hold values from 0.1 to 1.9
- out_first: bfloat16 [2048, 2048], P('tp', 'sp'), may hold values from -0.125 to 0.125
- pre_second: float32 [2048], replicated, may hold values from 0.1 to 1.9
- query_weight: bfloat16 [2048, 2048], P('sp', 'tp'), may hold values from -0.125 to 0.125
- key_weight: bfloat16 [2048, 2048], P('sp', 'tp'), may hold values from -0.125 to 0.125
- value_weight: bfloat16 [2048, 2048], P('sp', 'tp'), may hold values from -0.125 to 0.125
- rel_second: float32 [16, 257], P('tp'), may hold values from -4 to 4
- post_second: float32 [2048], replicated, may hold values from 0.1 to 1.9
- out_second: bfloat16 [2048, 2048], P('tp', 'sp'), may hold values from -0.125 to 0.125
Outputs:
- hidden_two: bfloat16 [2048, 2048], P(('grp', 'sp')), parts along dimension 0
The draws below stay inside these ranges and needn't reach their ends.
There are 2 independent parts, one for each index of `grp`. The reference program is written for one: setup_inputs(seed, part) draws one part's arguments, and reference() takes and returns one part's arrays. A program takes and returns all parts, laid end to end along the dimension named above; an argument that names none is the same for every part. Nothing has to cross between parts.
All inputs are finite; a program needn't handle non-finite values.
Results may differ from the reference program's by a relative error of at most 0.017.
Values may be sent and summed in bfloat16 or wider, within the bound.
A program may use at most 128 MiB of HBM per device.

```python
import jax
import jax.numpy as jnp
from jax import lax

D = 2048
HEADS = 16
SEG = 64
LEFT = 8
REACH = 512
REL_CLIP = 128
TOK_DEV = 128
TOKENS = 1024
N_SP = 8
N_TP = 2


def draw_pair(key):
    base = jax.random.fold_in(key, 41)
    key_draw = jnp.clip(jax.random.normal(jax.random.fold_in(base, 1), (TOKENS, D), jnp.float32), -6.0, 6.0)
    query_draw = jnp.clip(jax.random.normal(jax.random.fold_in(base, 2), (TOKENS, D), jnp.float32), -6.0, 6.0)
    return (query_draw, key_draw)


def draw_keys_first(key, part):
    return draw_pair(key)[1].astype(jnp.bfloat16)


def draw_queries_first(key, part):
    query_draw, key_draw = draw_pair(key)
    return query_draw.astype(jnp.bfloat16)


def block_levels(own_key, dims, cuts, smallest, top_value):
    def one(dim, parts):
        draws = jax.random.uniform(jax.random.fold_in(jax.random.fold_in(own_key, 6), dim), (parts,), jnp.float32, smallest / len(cuts), top_value / len(cuts))
        return jnp.repeat(jnp.exp(draws), dims[dim] // parts).reshape((-1,) + (1,) * (len(dims) - dim - 1))

    level = one(*cuts[0])
    for cut in cuts[1:]:
        level = level * one(*cut)
    return level


def normal_values(rng, shape, deviation, reach, shards=(), kind=jnp.bfloat16):
    values = jax.random.normal(rng, shape, jnp.float32) * deviation
    if len(shards) > 0:
        values = block_levels(rng, shape, shards, -0.22, 0.18) * values
    return jnp.clip(values, min=-reach, max=reach).astype(kind)


def setup_inputs(seed: int = 0, part: int = 0) -> dict:
    seeds = jax.random.split(jax.random.key(seed), 15)
    part_keys = jax.random.split(jax.random.fold_in(seeds[14], part), 15)
    return {
        "resid": normal_values(part_keys[0], (TOKENS, D), 1.0, 6.0, ((0, 8),)),
        "queries_first": draw_queries_first(jax.random.fold_in(jax.random.fold_in(seeds[14], part), 71), part),
        "keys_first": draw_keys_first(jax.random.fold_in(jax.random.fold_in(seeds[14], part), 71), part),
        "values_first": normal_values(part_keys[3], (TOKENS, D), 1.0, 6.0, ((0, 8), (1, 2))),
        "rel_first": normal_values(seeds[4], (HEADS, 2 * REL_CLIP + 1), 1.0, 4.0, ((0, 2),), jnp.float32),
        "post_first": jnp.clip(1.0 + 0.18 * jax.random.normal(seeds[5], (D,), jnp.float32), 0.1, 1.9),
        "out_first": normal_values(seeds[6], (D, D), D ** -0.5, 0.125, ((0, 2), (1, 8))),
        "pre_second": jnp.clip(1.0 + 0.18 * jax.random.normal(seeds[7], (D,), jnp.float32), 0.1, 1.9),
        "query_weight": normal_values(seeds[8], (D, D), D ** -0.5, 0.125, ((0, 8), (1, 2))),
        "key_weight": normal_values(seeds[9], (D, D), D ** -0.5, 0.125, ((0, 8), (1, 2))),
        "value_weight": normal_values(seeds[10], (D, D), D ** -0.5, 0.125, ((0, 8), (1, 2))),
        "rel_second": normal_values(seeds[11], (HEADS, 2 * REL_CLIP + 1), 1.0, 4.0, ((0, 2),), jnp.float32),
        "post_second": jnp.clip(1.0 + 0.18 * jax.random.normal(seeds[12], (D,), jnp.float32), 0.1, 1.9),
        "out_second": normal_values(seeds[13], (D, D), D ** -0.5, 0.125, ((0, 2), (1, 8))),
    }


EPS = 1e-06
NEG_FILL = -1e+30

def band_bias(bias_table):
    heads_here = bias_table.shape[0]
    band = (LEFT + 1) * SEG
    length = SEG + band
    index = jnp.arange(length, dtype=jnp.int32)
    distance = jnp.where(index < band, LEFT * SEG - index, LEFT * SEG + length - index)
    slot = jnp.clip(distance, -REL_CLIP, REL_CLIP) + REL_CLIP
    onehot = (slot[:, None] == jnp.arange(2 * REL_CLIP + 1, dtype=jnp.int32)[None, :]).astype(jnp.float32)
    diagonal_values = jnp.dot(bias_table, onehot.T, precision=lax.Precision.HIGHEST)
    spread = jnp.broadcast_to(diagonal_values[:, None, :], (heads_here, SEG, length)).reshape(heads_here, SEG * length)
    return spread[:, :SEG * (length - 1)].reshape(heads_here, SEG, length - 1)[:, :, :band]

def attend_band(queries, key_rows, value_rows, bias, key_live):
    rows, width = queries.shape
    heads_here = bias.shape[0]
    head_size = width // heads_here
    blocks = rows // SEG
    query_seg = queries.reshape(blocks, SEG, heads_here, head_size).astype(jnp.float32)
    key_seg = key_rows.reshape(blocks + LEFT, SEG, heads_here, head_size).astype(jnp.float32)
    value_seg = value_rows.reshape(blocks + LEFT, SEG, heads_here, head_size).astype(jnp.float32)
    live_seg = key_live.reshape(blocks + LEFT, SEG)
    key_band = jnp.concatenate([key_seg[earlier:earlier + blocks] for earlier in range(LEFT + 1)], axis=1)
    value_band = jnp.concatenate([value_seg[earlier:earlier + blocks] for earlier in range(LEFT + 1)], axis=1)
    live_band = jnp.concatenate([live_seg[earlier:earlier + blocks] for earlier in range(LEFT + 1)], axis=1)
    scores = jnp.einsum('nqhd,nkhd->nhqk', query_seg, key_band) * head_size ** (-0.5) + bias[None]
    scores = jnp.where(live_band[:, None, None, :], scores, NEG_FILL)
    largest = lax.optimization_barrier(jnp.max(scores, axis=-1, keepdims=True))
    weights = jnp.exp(scores - largest)
    weights = (weights / lax.optimization_barrier(jnp.sum(weights, axis=-1, keepdims=True))).astype(jnp.bfloat16)
    mixed = jnp.einsum('nhqk,nkhd->nqhd', weights.astype(jnp.float32), value_band)
    return mixed.astype(jnp.bfloat16).reshape(rows, width)

def attention_whole(queries, key_rows, value_rows, bias_table):
    bias = band_bias(bias_table)
    padding = jnp.zeros((REACH, key_rows.shape[1]), jnp.bfloat16)
    key_padded = jnp.concatenate([padding, key_rows], axis=0)
    value_padded = jnp.concatenate([padding, value_rows], axis=0)

    def one_block(number):
        start = (number * TOK_DEV).astype(jnp.int32)
        query_block = lax.dynamic_slice_in_dim(queries, start, TOK_DEV, 0)
        key_block = lax.dynamic_slice_in_dim(key_padded, start, TOK_DEV + REACH, 0)
        value_block = lax.dynamic_slice_in_dim(value_padded, start, TOK_DEV + REACH, 0)
        position = start - REACH + jnp.arange(TOK_DEV + REACH, dtype=jnp.int32)
        return attend_band(query_block, key_block, value_block, bias, position >= 0)
    result = lax.map(one_block, jnp.arange(N_SP, dtype=jnp.int32))
    return result.reshape(TOKENS, key_rows.shape[1])

def project_out(mixed, weight):
    width = D // N_TP
    total = jnp.zeros((mixed.shape[0], D), jnp.float32)
    for member in range(N_TP):
        term = jnp.dot(mixed[:, member * width:(member + 1) * width], weight[member * width:(member + 1) * width], preferred_element_type=jnp.float32).astype(jnp.bfloat16)
        total = total + term.astype(jnp.float32)
    return total.astype(jnp.bfloat16)

def normed(hidden, gain):
    values = hidden.astype(jnp.float32)
    scale = lax.rsqrt(lax.optimization_barrier(jnp.mean(values * values, axis=-1, keepdims=True)) + EPS)
    return (values * scale * gain).astype(jnp.bfloat16)

def residual_add(branch, residual, gain):
    values = branch.astype(jnp.float32)
    scale = lax.rsqrt(lax.optimization_barrier(jnp.mean(values * values, axis=-1, keepdims=True)) + EPS)
    return (residual.astype(jnp.float32) + values * scale * gain).astype(jnp.bfloat16)

def reference(resid, queries_first, keys_first, values_first, rel_first, post_first, out_first, pre_second, query_weight, key_weight, value_weight, rel_second, post_second, out_second):
    first = attention_whole(queries_first, keys_first, values_first, rel_first)
    hidden_one = residual_add(project_out(first, out_first), resid, post_first)
    inputs_two = normed(hidden_one, pre_second)
    queries_two = jnp.dot(inputs_two, query_weight, preferred_element_type=jnp.float32).astype(jnp.bfloat16)
    keys_two = jnp.dot(inputs_two, key_weight, preferred_element_type=jnp.float32).astype(jnp.bfloat16)
    values_two = jnp.dot(inputs_two, value_weight, preferred_element_type=jnp.float32).astype(jnp.bfloat16)
    second = attention_whole(queries_two, keys_two, values_two, rel_second)
    return residual_add(project_out(second, out_second), hidden_one, post_second)
```

```python
import jax
import jax.numpy as jnp
from jax import lax
from jax.experimental import pallas as pl
from jax.experimental.pallas import tpu as pltpu
from jax.sharding import PartitionSpec as P

MESH = pl.DeviceIdType.MESH
BF16 = jnp.bfloat16
F32 = jnp.float32

SEG = 64
LEFT = 8
REACH = 512
REL_CLIP = 128


EPS = 1e-06
NEG_FILL = -1e30


def from_behind(value, axis, steps):
    count = lax.axis_size(axis)
    initial, last = (max(0, -steps), min(count, count - steps))
    return lax.ppermute(value, axis, [(source, source + steps) for source in range(initial, last)])


def band_bias(bias_table):
    heads_here = bias_table.shape[0]
    band = (LEFT + 1) * SEG
    length = SEG + band
    index = jnp.arange(length, dtype=jnp.int32)
    distance = jnp.where(index < band, LEFT * SEG - index, LEFT * SEG + length - index)
    slot = jnp.clip(distance, -REL_CLIP, REL_CLIP) + REL_CLIP
    onehot = (slot[:, None] == jnp.arange(2 * REL_CLIP + 1, dtype=jnp.int32)[None, :]).astype(
        jnp.float32
    )
    diagonal_values = jnp.dot(bias_table, onehot.T, precision=lax.Precision.HIGHEST)
    spread = jnp.broadcast_to(diagonal_values[:, None, :], (heads_here, SEG, length)).reshape(
        heads_here, SEG * length
    )
    return spread[:, : SEG * (length - 1)].reshape(heads_here, SEG, length - 1)[:, :, :band]


def attend_band(queries, key_rows, value_rows, bias, key_live):
    rows, width = queries.shape
    heads_here = bias.shape[0]
    head_size = width // heads_here
    blocks = rows // SEG
    query_seg = queries.reshape(blocks, SEG, heads_here, head_size)
    key_seg = key_rows.reshape(blocks + LEFT, SEG, heads_here, head_size)
    value_seg = value_rows.reshape(blocks + LEFT, SEG, heads_here, head_size)
    live_seg = key_live.reshape(blocks + LEFT, SEG)
    key_band = jnp.concatenate(
        [key_seg[earlier : earlier + blocks] for earlier in range(LEFT + 1)], axis=1
    )
    value_band = jnp.concatenate(
        [value_seg[earlier : earlier + blocks] for earlier in range(LEFT + 1)], axis=1
    )
    live_band = jnp.concatenate(
        [live_seg[earlier : earlier + blocks] for earlier in range(LEFT + 1)], axis=1
    )
    scores = jnp.einsum("nqhd,nkhd->nhqk", query_seg, key_band, preferred_element_type=jnp.float32)
    scores = scores * head_size ** (-0.5) + bias[None]
    scores = jnp.where(live_band[:, None, None, :], scores, NEG_FILL)
    largest = jnp.max(scores, axis=-1, keepdims=True)
    weights = jnp.exp(scores - largest)
    weights = (weights / jnp.sum(weights, axis=-1, keepdims=True)).astype(jnp.bfloat16)
    mixed = jnp.einsum("nhqk,nkhd->nqhd", weights, value_band, preferred_element_type=jnp.float32)
    return mixed.astype(jnp.bfloat16).reshape(rows, width)


def extend_rows(pieces, member, own_rows):
    joined = jnp.concatenate([piece[member] for piece in pieces] + [own_rows], axis=0)
    return joined


def normed(hidden, gain):
    values = hidden.astype(jnp.float32)
    scale = lax.rsqrt(jnp.mean(values * values, axis=-1, keepdims=True) + EPS)
    return (values * scale * gain).astype(jnp.bfloat16)


def residual_add(branch, residual, gain):
    values = branch.astype(jnp.float32)
    scale = lax.rsqrt(jnp.mean(values * values, axis=-1, keepdims=True) + EPS)
    return (residual.astype(jnp.float32) + values * scale * gain).astype(jnp.bfloat16)


def combine(mixed, weight, residual, gain):
    partial_rows = jnp.dot(
        mixed, lax.all_gather(weight, "sp", axis=1, tiled=True), preferred_element_type=jnp.float32
    )
    branch = lax.psum_scatter(
        partial_rows.astype(jnp.bfloat16), "tp", scatter_dimension=0, tiled=True
    )
    return residual_add(branch, residual, gain)


def full_rows(share):
    return lax.all_gather(share, "tp", axis=0, tiled=True)


def shards(
    resid,
    queries_first,
    keys_first,
    values_first,
    rel_first,
    post_first,
    out_first,
    pre_second,
    query_weight,
    key_weight,
    value_weight,
    rel_second,
    post_second,
    out_second,
):
    tok_rows = resid.shape[0]
    n_sp = lax.axis_size("sp")
    if (
        rel_first.shape[0] == n_sp
        and n_sp % 2 == 0
        and lax.axis_size("tp") == 2
        and REACH % tok_rows == 0
        and tok_rows == REL_CLIP
    ):
        return by_heads(
            resid, queries_first, keys_first, values_first, rel_first, post_first, out_first,
            pre_second, query_weight, key_weight, value_weight, rel_second, post_second, out_second,
        )
    depth = (REACH + tok_rows - 1) // tok_rows
    anchor = lax.axis_index("sp") * tok_rows
    key_live = anchor - REACH + jnp.arange(tok_rows + REACH, dtype=jnp.int32) >= 0
    share_rows = tok_rows // lax.axis_size("tp")
    base_rows = lax.dynamic_slice_in_dim(resid, lax.axis_index("tp") * share_rows, share_rows, 0)
    earlier_first = [
        from_behind((keys_first, values_first), "sp", distance) for distance in range(depth, 0, -1)
    ]
    key_ext = extend_rows(earlier_first, 0, keys_first)
    value_ext = extend_rows(earlier_first, 1, values_first)
    first = attend_band(queries_first, key_ext, value_ext, band_bias(rel_first), key_live)
    hidden_one = combine(first, out_first, base_rows, post_first)
    inputs_two = full_rows(normed(hidden_one, pre_second))
    query_sum = jnp.dot(
        inputs_two,
        lax.all_gather(query_weight, "sp", axis=0, tiled=True),
        preferred_element_type=jnp.float32,
    )
    key_sum = jnp.dot(
        inputs_two,
        lax.all_gather(key_weight, "sp", axis=0, tiled=True),
        preferred_element_type=jnp.float32,
    )
    value_sum = jnp.dot(
        inputs_two,
        lax.all_gather(value_weight, "sp", axis=0, tiled=True),
        preferred_element_type=jnp.float32,
    )
    queries_two = query_sum.astype(jnp.bfloat16)
    keys_two = key_sum.astype(jnp.bfloat16)
    values_two = value_sum.astype(jnp.bfloat16)
    earlier_second = [
        from_behind((keys_two, values_two), "sp", distance) for distance in range(depth, 0, -1)
    ]
    key_ext_two = extend_rows(earlier_second, 0, keys_two)
    value_ext_two = extend_rows(earlier_second, 1, values_two)
    second = attend_band(queries_two, key_ext_two, value_ext_two, band_bias(rel_second), key_live)
    hidden_two = combine(second, out_second, hidden_one, post_second)
    return full_rows(hidden_two)


def scaled(values):
    return values * lax.rsqrt(jnp.mean(values * values, axis=-1, keepdims=True) + EPS)


def build_kernel(n, tok, head, width, reach):
    share = tok // 2
    cols = width // n
    span = reach + tok
    model = width

    def kernel(
        q_hbm, k_hbm, v_hbm, wq_hbm, wk_hbm, wv_hbm, resid_hbm, o1_hbm, o2_hbm,
        rel1, rel2, post1, pre2, post2,
        out_ref,
        heads, weights, outs, res, bias, mixed1, mixed2, parts1, parts2, branch1, branch2, rows2, last,
        loc_sem, hs, hr, ws, wr, fs, fr, gs, gr, bs, br, xs, xr, ys, yr,
    ):
        s = lax.axis_index("sp")
        t = lax.axis_index("tp")
        u = 1 - t
        side = s + 1 - 2 * lax.rem(s, 2)

        def rcopy(src, dst, ssem, rsem, sp, tp):
            return pltpu.make_async_remote_copy(
                src_ref=src, dst_ref=dst, send_sem=ssem, recv_sem=rsem,
                device_id={"sp": sp, "tp": tp}, device_id_type=MESH,
            )

        def peer(k):
            return lax.rem(s + k, n)

        barrier = pltpu.get_barrier_semaphore()
        for k in range(n):
            if k:
                pl.semaphore_signal(
                    barrier, inc=1, device_id={"sp": peer(k), "tp": t}, device_id_type=MESH
                )
            pl.semaphore_signal(
                barrier, inc=1, device_id={"sp": peer(k), "tp": u}, device_id_type=MESH
            )
        pl.semaphore_wait(barrier, 2 * n - 1)

        def lanes(j):
            return pl.ds(pl.multiple_of(j * head, head), head)

        def trows(j, base=0):
            return pl.ds(pl.multiple_of(base + j * tok, tok), tok)

        wrows = width // n

        def head_copy(i, ref, j, src):
            dst = heads.at[i, trows(src, reach)]
            return rcopy(ref.at[:, lanes(j)], dst, hs.at[i, j], hr.at[i, src], j, t)

        def weight_copy(i, ref, j, src):
            dst = weights.at[
                pl.ds(pl.multiple_of(src * wrows, wrows), wrows), pl.ds(i * head, head)
            ]
            return rcopy(ref.at[:, lanes(j)], dst, ws.at[i, j], wr.at[i, src], j, t)

        qkv = (q_hbm, k_hbm, v_hbm)
        wqkv = (wq_hbm, wk_hbm, wv_hbm)
        for k in range(1, n):
            for i in range(3):
                head_copy(i, qkv[i], peer(k), s).start()
        for i in range(3):
            pltpu.make_async_copy(
                qkv[i].at[:, lanes(s)], heads.at[i, trows(s, reach)], hr.at[i, s]
            ).start()
        for k in range(1, n):
            for i in range(3):
                weight_copy(i, wqkv[i], peer(k), s).start()
        for i in range(3):
            pltpu.make_async_copy(
                wqkv[i].at[:, lanes(s)],
                weights.at[pl.ds(pl.multiple_of(s * wrows, wrows), wrows), pl.ds(i * head, head)],
                wr.at[i, s],
            ).start()
        local = [
            pltpu.make_async_copy(o1_hbm, outs.at[0], loc_sem.at[0]),
            pltpu.make_async_copy(o2_hbm, outs.at[1], loc_sem.at[1]),
            pltpu.make_async_copy(
                resid_hbm.at[pl.ds(pl.multiple_of(t * share, share), share)], res, loc_sem.at[2]
            ),
        ]
        for copy in local:
            copy.start()

        near = 2 * REL_CLIP
        query = lax.broadcasted_iota(jnp.int32, (tok, span), 0) // SEG
        key = lax.broadcasted_iota(jnp.int32, (tok, span), 1) // SEG
        live = (key >= query) & (key <= query + LEFT)
        for layer, rel in enumerate((rel1, rel2)):
            line = rel[pl.ds(s, 1), :]
            spread = jnp.broadcast_to(line, (tok, line.shape[1]))
            row = lax.broadcasted_iota(jnp.int32, spread.shape, 0)
            step = 1
            while step < tok:
                moved = pltpu.roll(spread, step, 1)
                spread = jnp.where(lax.rem(row // step, 2) == 1, moved, spread)
                step *= 2
            far = jnp.broadcast_to(line[:, near : near + 1], (tok, span - near))
            whole = jnp.concatenate([far, spread[:, :near]], axis=1)
            bias[layer] = jnp.where(live, whole, NEG_FILL)

        heads[1, :reach] = jnp.zeros((reach, head), BF16)
        heads[2, :reach] = jnp.zeros((reach, head), BF16)

        def attend(layer, b):
            q = heads[0, trows(b, reach)]
            k = heads[1, pl.ds(pl.multiple_of(b * tok, tok), span)]
            v = heads[2, pl.ds(pl.multiple_of(b * tok, tok), span)]
            scores = lax.dot_general(
                q, k, (((1,), (1,)), ((), ())), preferred_element_type=F32
            ) * head ** (-0.5) + bias[layer]
            column = lax.broadcasted_iota(jnp.int32, scores.shape, 1)
            scores = jnp.where(column >= reach - b * tok, scores, NEG_FILL)
            e = jnp.exp(scores - jnp.max(scores, axis=-1, keepdims=True))
            e = (e * (1.0 / jnp.sum(e, axis=-1, keepdims=True))).astype(BF16)
            return jnp.dot(e, v, preferred_element_type=F32).astype(BF16)

        def layer_branch(layer, mixed, parts, branch, ms, mr, ps, pr, wait_block):
            def mcopy(b, src, k, sp):
                block = mixed.at[src, trows(b)]
                return rcopy(block, block, ms.at[b, k], mr.at[b, src], sp, t)

            half = n // 2

            def own(b, _):
                wait_block(b)
                mixed[s, trows(b)] = attend(layer, b)
                mcopy(b, s, 0, side).start()
                for k in range(1, half):
                    mcopy(b, s, k, peer(2 * k)).start()
                return 0

            lax.fori_loop(0, n, own, 0)

            def pcopy(b, c):
                return rcopy(
                    parts.at[b, c], branch.at[t, s], ps.at[b, c], pr.at[t, s], b, c
                )

            def forward(b):
                for k in range(1, half):
                    mcopy(b, peer(2 * k), k, side).wait_recv()
                    mcopy(b, peer(2 * k), half - 1 + k, side).start()

            def project(b):
                for k in range(half):
                    mcopy(b, lax.rem(side + 2 * k, n), k, side).wait_recv()
                lhs = jnp.concatenate([mixed[j, trows(b)] for j in range(n)], axis=1)
                part = jnp.dot(lhs, outs[layer], preferred_element_type=F32).astype(BF16)
                parts[b, 0] = part[:share]
                parts[b, 1] = part[share:]
                pcopy(b, u).start()

                @pl.when(b != s)
                def _():
                    pcopy(b, t).start()

                @pl.when(b == s)
                def _():
                    pltpu.make_async_copy(
                        parts.at[b, t], branch.at[t, s], pr.at[t, s]
                    ).start()

            def step(b, _):
                forward(b)

                @pl.when(b > 0)
                def _():
                    project(b - 1)

                return 0

            lax.fori_loop(0, n, step, 0)
            project(n - 1)

            def arrived(j, _):
                for c in range(2):
                    rcopy(
                        parts.at[0, 0], branch.at[c, j], ps.at[0, 0], pr.at[c, j], side, t
                    ).wait_recv()
                return 0

            lax.fori_loop(0, n, arrived, 0)

            def drain(b, _):
                for k in range(2 * half - 1):
                    mcopy(b, s, k, side).wait_send()
                pcopy(b, u).wait_send()

                @pl.when(b != s)
                def _():
                    pcopy(b, t).wait_send()

                return 0

            total = [
                jnp.concatenate([branch[c, j] for j in range(n)], axis=1).astype(F32)
                for c in range(2)
            ]
            return (total[0] + total[1]).astype(BF16).astype(F32), drain

        def heads_ready(b):
            for i in range(3):
                head_copy(i, qkv[i], side, b).wait_recv()

        local[0].wait()
        local[1].wait()
        values, drain1 = layer_branch(
            0, mixed1, parts1, branch1, fs, fr, bs.at[0], br.at[0], heads_ready
        )
        local[2].wait()
        hidden = (res[...].astype(F32) + scaled(values) * post1[...]).astype(BF16)
        res[...] = hidden
        rows2[2 * s + t] = (scaled(hidden.astype(F32)) * pre2[...]).astype(BF16)

        def xcopy(src, c, k, sp, tp):
            block = rows2.at[2 * src + c]
            return rcopy(block, block, xs.at[src, k], xr.at[2 * src + c], sp, tp)

        half = n // 2
        xcopy(s, t, 0, side, t).start()
        for k in range(1, half):
            xcopy(s, t, k + 1, peer(2 * k), t).start()
        xcopy(s, t, 1, s, u).start()
        for k in range(1, half):
            src = peer(2 * k)
            xcopy(src, t, 0, side, t).wait_recv()
            xcopy(src, t, 0, side, t).start()
            xcopy(src, t, 1, s, u).start()

        def weights_ready(j, _):
            for i in range(3):
                weight_copy(i, wqkv[i], side, j).wait_recv()
            return 0

        lax.fori_loop(0, n, weights_ready, 0)

        def project_rows(src):
            xcopy(src, u, 1, s, u).wait_recv()
            lhs = rows2[pl.ds(2 * src, 2)].reshape(tok, model)
            got = jnp.dot(lhs, weights[...], preferred_element_type=F32).astype(BF16)
            for i in range(3):
                heads[i, trows(src, reach)] = got[:, i * head : (i + 1) * head]

        def near_rows(k, _):
            src = lax.rem(side + 2 * k, n)
            xcopy(src, t, 0, side, t).wait_recv()
            xcopy(src, t, 1, s, u).start()
            project_rows(lax.rem(s + 2 * k, n))
            return 0

        lax.fori_loop(0, half, near_rows, 0)

        def far_rows(k, _):
            project_rows(lax.rem(side + 2 * k, n))
            return 0

        lax.fori_loop(0, half, far_rows, 0)

        values, drain2 = layer_branch(
            1, mixed2, parts2, branch2, gs, gr, bs.at[1], br.at[1], lambda b: None
        )
        done = (res[...].astype(F32) + scaled(values) * post2[...]).astype(BF16)
        last[t] = done
        final = rcopy(last.at[t], last.at[t], ys, yr, s, u)
        final.start()

        lax.fori_loop(0, n, lambda b, c: drain1(b, c), 0)
        lax.fori_loop(0, n, lambda b, c: drain2(b, c), 0)
        for k in range(1, n):
            for i in range(3):
                head_copy(i, qkv[i], peer(k), s).wait_send()
                weight_copy(i, wqkv[i], peer(k), s).wait_send()
        for k in range(half + 1):
            xcopy(s, t, k, side, t).wait_send()
        for k in range(1, half):
            xcopy(peer(2 * k), t, 0, side, t).wait_send()
            xcopy(peer(2 * k), t, 1, side, t).wait_send()
        for k in range(half):
            xcopy(lax.rem(side + 2 * k, n), t, 1, side, t).wait_send()
        final.wait_send()
        rcopy(last.at[u], last.at[u], ys, yr, s, u).wait_recv()
        out_ref[:share] = last[0]
        out_ref[share:] = last[1]

    half = n // 2
    scratch = [
        pltpu.VMEM((3, reach + n * tok, head), BF16),
        pltpu.VMEM((width, 3 * head), BF16),
        pltpu.VMEM((2, n * head, cols), BF16),
        pltpu.VMEM((share, width), BF16),
        pltpu.VMEM((2, tok, span), F32),
        pltpu.VMEM((n, n * tok, head), BF16),
        pltpu.VMEM((n, n * tok, head), BF16),
        pltpu.VMEM((n, 2, share, cols), BF16),
        pltpu.VMEM((n, 2, share, cols), BF16),
        pltpu.VMEM((2, n, share, cols), BF16),
        pltpu.VMEM((2, n, share, cols), BF16),
        pltpu.VMEM((2 * n, share, width), BF16),
        pltpu.VMEM((2, share, width), BF16),
        pltpu.SemaphoreType.DMA((3,)),
        pltpu.SemaphoreType.DMA((3, n)),
        pltpu.SemaphoreType.DMA((3, n)),
        pltpu.SemaphoreType.DMA((3, n)),
        pltpu.SemaphoreType.DMA((3, n)),
        pltpu.SemaphoreType.DMA((n, 2 * half - 1)),
        pltpu.SemaphoreType.DMA((n, n)),
        pltpu.SemaphoreType.DMA((n, 2 * half - 1)),
        pltpu.SemaphoreType.DMA((n, n)),
        pltpu.SemaphoreType.DMA((2, n, 2)),
        pltpu.SemaphoreType.DMA((2, 2, n)),
        pltpu.SemaphoreType.DMA((n, half + 1)),
        pltpu.SemaphoreType.DMA((2 * n,)),
        pltpu.SemaphoreType.DMA,
        pltpu.SemaphoreType.DMA,
    ]
    return kernel, scratch


def reversed_line(table, tok):
    top = table[:, -1:]
    return jnp.concatenate(
        [table[:, :0:-1], jnp.broadcast_to(top, (table.shape[0], tok))], axis=1
    )


def by_heads(
    resid, queries_first, keys_first, values_first, rel_first, post_first, out_first, pre_second,
    query_weight, key_weight, value_weight, rel_second, post_second, out_second,
):
    n = lax.axis_size("sp")
    tok, width = resid.shape
    head = queries_first.shape[1] // rel_first.shape[0]
    kernel, scratch = build_kernel(n, tok, head, width, REACH)
    hbm = pl.BlockSpec(memory_space=pl.ANY)
    vmem = pl.BlockSpec(memory_space=pltpu.VMEM)
    return pl.pallas_call(
        kernel,
        out_shape=jax.ShapeDtypeStruct((tok, width), BF16),
        in_specs=[hbm] * 9 + [vmem] * 5,
        out_specs=vmem,
        scratch_shapes=scratch,
        compiler_params=pltpu.CompilerParams(
            collective_id=0, has_side_effects=True, vmem_limit_bytes=40 * 2**20
        ),
    )(
        queries_first, keys_first, values_first, query_weight, key_weight, value_weight, resid,
        out_first, out_second, reversed_line(rel_first, tok), reversed_line(rel_second, tok),
        post_first[None], pre_second[None], post_second[None],
    )


def solution(mesh):
    in_specs = (
        P(("grp", "sp"), None),
        P(("grp", "sp"), "tp"),
        P(("grp", "sp"), "tp"),
        P(("grp", "sp"), "tp"),
        P("tp", None),
        P(),
        P("tp", "sp"),
        P(),
        P("sp", "tp"),
        P("sp", "tp"),
        P("sp", "tp"),
        P("tp", None),
        P(),
        P("tp", "sp"),
    )
    out_specs = P(("grp", "sp"), None)
    return jax.shard_map(shards, mesh=mesh, in_specs=in_specs, out_specs=out_specs, check_vma=False)
```

```python
import jax
import jax.numpy as jnp
from jax import lax
from jax.experimental import pallas as pl
from jax.experimental.pallas import tpu as pltpu
from jax.sharding import PartitionSpec as P

MESH = pl.DeviceIdType.MESH
BF16 = jnp.bfloat16
F32 = jnp.float32

SEG = 64
LEFT = 8
REACH = 512
REL_CLIP = 128


EPS = 1e-06
NEG_FILL = -1e30


def from_behind(value, axis, steps):
    count = lax.axis_size(axis)
    initial, last = (max(0, -steps), min(count, count - steps))
    return lax.ppermute(value, axis, [(source, source + steps) for source in range(initial, last)])


def band_bias(bias_table):
    heads_here = bias_table.shape[0]
    band = (LEFT + 1) * SEG
    length = SEG + band
    index = jnp.arange(length, dtype=jnp.int32)
    distance = jnp.where(index < band, LEFT * SEG - index, LEFT * SEG + length - index)
    slot = jnp.clip(distance, -REL_CLIP, REL_CLIP) + REL_CLIP
    onehot = (slot[:, None] == jnp.arange(2 * REL_CLIP + 1, dtype=jnp.int32)[None, :]).astype(
        jnp.float32
    )
    diagonal_values = jnp.dot(bias_table, onehot.T, precision=lax.Precision.HIGHEST)
    spread = jnp.broadcast_to(diagonal_values[:, None, :], (heads_here, SEG, length)).reshape(
        heads_here, SEG * length
    )
    return spread[:, : SEG * (length - 1)].reshape(heads_here, SEG, length - 1)[:, :, :band]


def attend_band(queries, key_rows, value_rows, bias, key_live):
    rows, width = queries.shape
    heads_here = bias.shape[0]
    head_size = width // heads_here
    blocks = rows // SEG
    query_seg = queries.reshape(blocks, SEG, heads_here, head_size)
    key_seg = key_rows.reshape(blocks + LEFT, SEG, heads_here, head_size)
    value_seg = value_rows.reshape(blocks + LEFT, SEG, heads_here, head_size)
    live_seg = key_live.reshape(blocks + LEFT, SEG)
    key_band = jnp.concatenate(
        [key_seg[earlier : earlier + blocks] for earlier in range(LEFT + 1)], axis=1
    )
    value_band = jnp.concatenate(
        [value_seg[earlier : earlier + blocks] for earlier in range(LEFT + 1)], axis=1
    )
    live_band = jnp.concatenate(
        [live_seg[earlier : earlier + blocks] for earlier in range(LEFT + 1)], axis=1
    )
    scores = jnp.einsum("nqhd,nkhd->nhqk", query_seg, key_band, preferred_element_type=jnp.float32)
    scores = scores * head_size ** (-0.5) + bias[None]
    scores = jnp.where(live_band[:, None, None, :], scores, NEG_FILL)
    largest = jnp.max(scores, axis=-1, keepdims=True)
    weights = jnp.exp(scores - largest)
    weights = (weights / jnp.sum(weights, axis=-1, keepdims=True)).astype(jnp.bfloat16)
    mixed = jnp.einsum("nhqk,nkhd->nqhd", weights, value_band, preferred_element_type=jnp.float32)
    return mixed.astype(jnp.bfloat16).reshape(rows, width)


def extend_rows(pieces, member, own_rows):
    joined = jnp.concatenate([piece[member] for piece in pieces] + [own_rows], axis=0)
    return joined


def normed(hidden, gain):
    values = hidden.astype(jnp.float32)
    scale = lax.rsqrt(jnp.mean(values * values, axis=-1, keepdims=True) + EPS)
    return (values * scale * gain).astype(jnp.bfloat16)


def residual_add(branch, residual, gain):
    values = branch.astype(jnp.float32)
    scale = lax.rsqrt(jnp.mean(values * values, axis=-1, keepdims=True) + EPS)
    return (residual.astype(jnp.float32) + values * scale * gain).astype(jnp.bfloat16)


def combine(mixed, weight, residual, gain):
    partial_rows = jnp.dot(
        mixed, lax.all_gather(weight, "sp", axis=1, tiled=True), preferred_element_type=jnp.float32
    )
    branch = lax.psum_scatter(
        partial_rows.astype(jnp.bfloat16), "tp", scatter_dimension=0, tiled=True
    )
    return residual_add(branch, residual, gain)


def full_rows(share):
    return lax.all_gather(share, "tp", axis=0, tiled=True)


def shards(
    resid,
    queries_first,
    keys_first,
    values_first,
    rel_first,
    post_first,
    out_first,
    pre_second,
    query_weight,
    key_weight,
    value_weight,
    rel_second,
    post_second,
    out_second,
):
    tok_rows = resid.shape[0]
    n_sp = lax.axis_size("sp")
    if (
        rel_first.shape[0] == n_sp
        and n_sp % 2 == 0
        and lax.axis_size("tp") == 2
        and lax.axis_size("grp") == 2
        and REACH % tok_rows == 0
        and tok_rows == REL_CLIP
    ):
        return by_heads(
            resid, queries_first, keys_first, values_first, rel_first, post_first, out_first,
            pre_second, query_weight, key_weight, value_weight, rel_second, post_second, out_second,
        )
    depth = (REACH + tok_rows - 1) // tok_rows
    anchor = lax.axis_index("sp") * tok_rows
    key_live = anchor - REACH + jnp.arange(tok_rows + REACH, dtype=jnp.int32) >= 0
    share_rows = tok_rows // lax.axis_size("tp")
    base_rows = lax.dynamic_slice_in_dim(resid, lax.axis_index("tp") * share_rows, share_rows, 0)
    earlier_first = [
        from_behind((keys_first, values_first), "sp", distance) for distance in range(depth, 0, -1)
    ]
    key_ext = extend_rows(earlier_first, 0, keys_first)
    value_ext = extend_rows(earlier_first, 1, values_first)
    first = attend_band(queries_first, key_ext, value_ext, band_bias(rel_first), key_live)
    hidden_one = combine(first, out_first, base_rows, post_first)
    inputs_two = full_rows(normed(hidden_one, pre_second))
    query_sum = jnp.dot(
        inputs_two,
        lax.all_gather(query_weight, "sp", axis=0, tiled=True),
        preferred_element_type=jnp.float32,
    )
    key_sum = jnp.dot(
        inputs_two,
        lax.all_gather(key_weight, "sp", axis=0, tiled=True),
        preferred_element_type=jnp.float32,
    )
    value_sum = jnp.dot(
        inputs_two,
        lax.all_gather(value_weight, "sp", axis=0, tiled=True),
        preferred_element_type=jnp.float32,
    )
    queries_two = query_sum.astype(jnp.bfloat16)
    keys_two = key_sum.astype(jnp.bfloat16)
    values_two = value_sum.astype(jnp.bfloat16)
    earlier_second = [
        from_behind((keys_two, values_two), "sp", distance) for distance in range(depth, 0, -1)
    ]
    key_ext_two = extend_rows(earlier_second, 0, keys_two)
    value_ext_two = extend_rows(earlier_second, 1, values_two)
    second = attend_band(queries_two, key_ext_two, value_ext_two, band_bias(rel_second), key_live)
    hidden_two = combine(second, out_second, hidden_one, post_second)
    return full_rows(hidden_two)


def scaled(values):
    return values * lax.rsqrt(jnp.mean(values * values, axis=-1, keepdims=True) + EPS)


def build_kernel(n, tok, head, width, reach):
    share = tok // 2
    cols = width // n
    span = reach + tok
    model = width

    def kernel(
        q_hbm, k_hbm, v_hbm, wq_hbm, wk_hbm, wv_hbm, resid_hbm, o1_hbm, o2_hbm,
        rel1, rel2, post1, pre2, post2,
        out_ref,
        heads, weights, outs, res, bias, mixed1, mixed2, parts, inbox, joined, branch, rows2, last,
        loc_sem, hs, hr, ws, wr, wf, fs, fr, gs, gr, ps, pr, bs, br, xs, xr, ys, yr,
    ):
        s = lax.axis_index("sp")
        t = lax.axis_index("tp")
        g = lax.axis_index("grp")
        u = 1 - t
        side = s + 1 - 2 * lax.rem(s, 2)

        def rcopy(src, dst, ssem, rsem, sp, tp, grp=g):
            return pltpu.make_async_remote_copy(
                src_ref=src, dst_ref=dst, send_sem=ssem, recv_sem=rsem,
                device_id={"grp": grp, "sp": sp, "tp": tp}, device_id_type=MESH,
            )

        def peer(k):
            return lax.rem(s + k, n)

        barrier = pltpu.get_barrier_semaphore()
        for k in range(n):
            if k:
                pl.semaphore_signal(
                    barrier, inc=1, device_id={"sp": peer(k), "tp": t}, device_id_type=MESH
                )
            pl.semaphore_signal(
                barrier, inc=1, device_id={"sp": peer(k), "tp": u}, device_id_type=MESH
            )
        pl.semaphore_signal(
            barrier, inc=1, device_id={"grp": 1 - g, "sp": s, "tp": t}, device_id_type=MESH
        )
        pl.semaphore_wait(barrier, 2 * n)

        def lanes(j):
            return pl.ds(pl.multiple_of(j * head, head), head)

        def trows(j, base=0):
            return pl.ds(pl.multiple_of(base + j * tok, tok), tok)

        wrows = width // n

        def head_copy(i, ref, j, src):
            dst = heads.at[i, trows(src, reach)]
            return rcopy(ref.at[:, lanes(j)], dst, hs.at[i, j], hr.at[i, src], j, t)

        hrows = wrows // 2

        def weight_half(i, src, part):
            start = pl.multiple_of(src * wrows + part * hrows, hrows)
            return weights.at[pl.ds(start, hrows), pl.ds(i * head, head)]

        def weight_copy(i, j, src):
            piece = wqkv[i].at[pl.ds(pl.multiple_of(g * hrows, hrows), hrows), lanes(j)]
            return rcopy(piece, weight_half(i, src, g), ws.at[i, j], wr.at[i, src, g], j, t)

        def weight_hand(i, src):
            piece = weight_half(i, src, g)
            return rcopy(piece, piece, wf.at[i, src], wr.at[i, src, g], s, t, 1 - g)

        def weight_handed(i, src):
            piece = weight_half(i, src, 1 - g)
            return rcopy(piece, piece, wf.at[i, src], wr.at[i, src, 1 - g], s, t, 1 - g)

        def own_weights(i):
            return pltpu.make_async_copy(
                wqkv[i].at[:, lanes(s)],
                weights.at[pl.ds(pl.multiple_of(s * wrows, wrows), wrows), pl.ds(i * head, head)],
                wr.at[i, s, 0],
            )

        qkv = (q_hbm, k_hbm, v_hbm)
        wqkv = (wq_hbm, wk_hbm, wv_hbm)
        for k in range(1, n):
            for i in range(3):
                head_copy(i, qkv[i], peer(k), s).start()
        for i in range(3):
            pltpu.make_async_copy(
                qkv[i].at[:, lanes(s)], heads.at[i, trows(s, reach)], hr.at[i, s]
            ).start()
        for i in range(3):
            own_weights(i).start()

        def send_weights():
            for i in range(3):
                for k in range(1, n):
                    weight_copy(i, peer(k), s).start()

        local = [
            pltpu.make_async_copy(o1_hbm, outs.at[0], loc_sem.at[0]),
            pltpu.make_async_copy(o2_hbm, outs.at[1], loc_sem.at[1]),
            pltpu.make_async_copy(
                resid_hbm.at[pl.ds(pl.multiple_of(t * share, share), share)], res, loc_sem.at[2]
            ),
        ]
        for copy in local:
            copy.start()

        near = 2 * REL_CLIP
        query = lax.broadcasted_iota(jnp.int32, (tok, span), 0) // SEG
        key = lax.broadcasted_iota(jnp.int32, (tok, span), 1) // SEG
        live = (key >= query) & (key <= query + LEFT)
        for layer, rel in enumerate((rel1, rel2)):
            table = rel[pl.ds(s, 1), :]
            top = table[:, near : near + 1]
            entry = lax.broadcasted_iota(jnp.int32, (near, near + tok), 0)
            place = lax.broadcasted_iota(jnp.int32, (near, near + tok), 1)
            flip = (entry + place == near).astype(F32)
            line = jnp.dot(
                jnp.broadcast_to(table[:, :near], (8, near)), flip,
                preferred_element_type=F32, precision=lax.Precision.HIGHEST,
            )[:1]
            spot = lax.broadcasted_iota(jnp.int32, line.shape, 1)
            line = jnp.where((spot == 0) | (spot >= near), top, line)
            spread = jnp.broadcast_to(line, (tok, near + tok))
            row = lax.broadcasted_iota(jnp.int32, spread.shape, 0)
            step = 1
            while step < tok:
                moved = pltpu.roll(spread, step, 1)
                spread = jnp.where(lax.rem(row // step, 2) == 1, moved, spread)
                step *= 2
            far = jnp.broadcast_to(top, (tok, span - near))
            whole = jnp.concatenate([far, spread[:, :near]], axis=1)
            bias[layer] = jnp.where(live, whole, NEG_FILL)

        heads[1, :reach] = jnp.zeros((reach, head), BF16)
        heads[2, :reach] = jnp.zeros((reach, head), BF16)

        def attend(layer, b):
            q = heads[0, trows(b, reach)]
            k = heads[1, pl.ds(pl.multiple_of(b * tok, tok), span)]
            v = heads[2, pl.ds(pl.multiple_of(b * tok, tok), span)]
            scores = lax.dot_general(
                q, k, (((1,), (1,)), ((), ())), preferred_element_type=F32
            ) * head ** (-0.5) + bias[layer]
            column = lax.broadcasted_iota(jnp.int32, scores.shape, 1)
            scores = jnp.where(column >= reach - b * tok, scores, NEG_FILL)
            e = jnp.exp(scores - jnp.max(scores, axis=-1, keepdims=True))
            e = (e * (1.0 / jnp.sum(e, axis=-1, keepdims=True))).astype(BF16)
            return jnp.dot(e, v, preferred_element_type=F32).astype(BF16)

        def layer_branch(layer, mixed, ms, mr, wait_block, after_own):
            def mcopy(b, src, k, sp):
                block = mixed.at[src, trows(b)]
                return rcopy(block, block, ms.at[b, k], mr.at[b, src], sp, t)

            half = n // 2

            def own(b, _):
                wait_block(b)
                mixed[s, trows(b)] = attend(layer, b)
                mcopy(b, s, 0, side).start()
                for k in range(1, half):
                    mcopy(b, s, k, peer(2 * k)).start()
                return 0

            lax.fori_loop(0, n, own, 0)
            after_own()

            def pcopy(b):
                return rcopy(
                    parts.at[layer, b, u], inbox.at[layer, b],
                    ps.at[layer, b], pr.at[layer, b], s, u,
                )

            def bcopy(b, src):
                return rcopy(
                    joined.at[layer, b], branch.at[layer, src],
                    bs.at[layer, b], br.at[layer, src], b, t,
                )

            def forward(b):
                for k in range(1, half):
                    mcopy(b, peer(2 * k), k, side).wait_recv()
                    mcopy(b, peer(2 * k), half - 1 + k, side).start()

            def project(b):
                for k in range(half):
                    mcopy(b, lax.rem(side + 2 * k, n), k, side).wait_recv()
                lhs = jnp.concatenate([mixed[j, trows(b)] for j in range(n)], axis=1)
                part = jnp.dot(lhs, outs[layer], preferred_element_type=F32).astype(BF16)
                parts[layer, b, 0] = part[:share]
                parts[layer, b, 1] = part[share:]
                pcopy(b).start()

            def join(b):
                pcopy(b).wait_recv()
                total = parts[layer, b, t].astype(F32) + inbox[layer, b].astype(F32)
                joined[layer, b] = total.astype(BF16)

                @pl.when(b != s)
                def _():
                    bcopy(b, s).start()

                @pl.when(b == s)
                def _():
                    pltpu.make_async_copy(
                        joined.at[layer, b], branch.at[layer, s], br.at[layer, s]
                    ).start()

            def step(b, _):
                forward(b)

                @pl.when(b > 0)
                def _():
                    project(b - 1)

                @pl.when(b > 1)
                def _():
                    join(b - 2)

                return 0

            lax.fori_loop(0, n, step, 0)
            project(n - 1)
            join(n - 2)
            join(n - 1)

            def arrived(j, _):
                bcopy(side, j).wait_recv()
                return 0

            lax.fori_loop(0, n, arrived, 0)

            def drain(b, _):
                for k in range(2 * half - 1):
                    mcopy(b, s, k, side).wait_send()
                pcopy(b).wait_send()

                @pl.when(b != s)
                def _():
                    bcopy(b, s).wait_send()

                return 0

            values = jnp.concatenate([branch[layer, j] for j in range(n)], axis=1)
            return values.astype(F32), drain

        def heads_ready(b):
            for i in range(3):
                head_copy(i, qkv[i], side, b).wait_recv()

        local[0].wait()
        local[1].wait()
        values, drain1 = layer_branch(0, mixed1, fs, fr, heads_ready, send_weights)
        local[2].wait()
        hidden = (res[...].astype(F32) + scaled(values) * post1[...]).astype(BF16)
        res[...] = hidden
        rows2[2 * s + t] = (scaled(hidden.astype(F32)) * pre2[...]).astype(BF16)

        half = n // 2
        wide = width // half

        def xcopy(src, c, k, sp, tp, m):
            block = rows2.at[2 * src + c, :, pl.ds(pl.multiple_of(m * wide, wide), wide)]
            return rcopy(block, block, xs.at[src, k, m], xr.at[2 * src + c, m], sp, tp)

        def xsend(m, _):
            for k in range(1, half):
                xcopy(s, t, k + 1, peer(2 * k), t, m).start()
            xcopy(s, t, 0, side, t, m).start()
            xcopy(s, t, 1, s, u, m).start()
            return 0

        lax.fori_loop(0, half, xsend, 0)

        def hand_weights(k, _):
            for i in range(3):
                weight_copy(i, side, peer(k)).wait_recv()
                weight_hand(i, peer(k)).start()
            return 0

        lax.fori_loop(1, n, hand_weights, 0)

        def near_rows(m, _):
            for k in range(1, half):
                src = peer(2 * k)
                xcopy(src, t, 0, side, t, m).wait_recv()
                xcopy(src, t, 0, side, t, m).start()
                xcopy(src, t, 1, s, u, m).start()
            return 0

        lax.fori_loop(0, half, near_rows, 0)

        def weights_ready(k, _):
            for i in range(3):
                weight_handed(i, peer(k)).wait_recv()
            return 0

        lax.fori_loop(1, n, weights_ready, 0)
        for i in range(3):
            own_weights(i).wait()

        def project_rows(src):
            for m in range(half):
                xcopy(src, u, 1, s, u, m).wait_recv()
            lhs = rows2[pl.ds(2 * src, 2)].reshape(tok, model)
            got = jnp.dot(lhs, weights[...], preferred_element_type=F32).astype(BF16)
            for i in range(3):
                heads[i, trows(src, reach)] = got[:, i * head : (i + 1) * head]

        def far_rows(m, _):
            for k in range(half):
                src = lax.rem(side + 2 * k, n)
                xcopy(src, t, 0, side, t, m).wait_recv()
                xcopy(src, t, 1, s, u, m).start()
            project_rows(peer(2 * m))
            return 0

        lax.fori_loop(0, half, far_rows, 0)

        def last_rows(k, _):
            project_rows(lax.rem(side + 2 * k, n))
            return 0

        lax.fori_loop(0, half, last_rows, 0)

        values, drain2 = layer_branch(1, mixed2, gs, gr, lambda b: None, lambda: None)
        done = (res[...].astype(F32) + scaled(values) * post2[...]).astype(BF16)
        last[t] = done
        final = rcopy(last.at[t], last.at[t], ys, yr, s, u)
        final.start()

        lax.fori_loop(0, n, lambda b, c: drain1(b, c), 0)
        lax.fori_loop(0, n, lambda b, c: drain2(b, c), 0)
        def drain_first(k, _):
            for i in range(3):
                head_copy(i, qkv[i], peer(k), s).wait_send()
                weight_copy(i, peer(k), s).wait_send()
                weight_hand(i, peer(k)).wait_send()
            return 0

        lax.fori_loop(1, n, drain_first, 0)

        def drain_rows(m, _):
            for k in range(half + 1):
                xcopy(s, t, k, side, t, m).wait_send()
            for k in range(1, half):
                xcopy(peer(2 * k), t, 0, side, t, m).wait_send()
                xcopy(peer(2 * k), t, 1, side, t, m).wait_send()
            for k in range(half):
                xcopy(lax.rem(side + 2 * k, n), t, 1, side, t, m).wait_send()
            return 0

        lax.fori_loop(0, half, drain_rows, 0)
        final.wait_send()
        rcopy(last.at[u], last.at[u], ys, yr, s, u).wait_recv()
        out_ref[:share] = last[0]
        out_ref[share:] = last[1]

    half = n // 2
    scratch = [
        pltpu.VMEM((3, reach + n * tok, head), BF16),
        pltpu.VMEM((width, 3 * head), BF16),
        pltpu.VMEM((2, n * head, cols), BF16),
        pltpu.VMEM((share, width), BF16),
        pltpu.VMEM((2, tok, span), F32),
        pltpu.VMEM((n, n * tok, head), BF16),
        pltpu.VMEM((n, n * tok, head), BF16),
        pltpu.VMEM((2, n, 2, share, cols), BF16),
        pltpu.VMEM((2, n, share, cols), BF16),
        pltpu.VMEM((2, n, share, cols), BF16),
        pltpu.VMEM((2, n, share, cols), BF16),
        pltpu.VMEM((2 * n, share, width), BF16),
        pltpu.VMEM((2, share, width), BF16),
        pltpu.SemaphoreType.DMA((3,)),
        pltpu.SemaphoreType.DMA((3, n)),
        pltpu.SemaphoreType.DMA((3, n)),
        pltpu.SemaphoreType.DMA((3, n)),
        pltpu.SemaphoreType.DMA((3, n, 2)),
        pltpu.SemaphoreType.DMA((3, n)),
        pltpu.SemaphoreType.DMA((n, 2 * half - 1)),
        pltpu.SemaphoreType.DMA((n, n)),
        pltpu.SemaphoreType.DMA((n, 2 * half - 1)),
        pltpu.SemaphoreType.DMA((n, n)),
        pltpu.SemaphoreType.DMA((2, n)),
        pltpu.SemaphoreType.DMA((2, n)),
        pltpu.SemaphoreType.DMA((2, n)),
        pltpu.SemaphoreType.DMA((2, n)),
        pltpu.SemaphoreType.DMA((n, half + 1, half)),
        pltpu.SemaphoreType.DMA((2 * n, half)),
        pltpu.SemaphoreType.DMA,
        pltpu.SemaphoreType.DMA,
    ]
    return kernel, scratch


def by_heads(
    resid, queries_first, keys_first, values_first, rel_first, post_first, out_first, pre_second,
    query_weight, key_weight, value_weight, rel_second, post_second, out_second,
):
    n = lax.axis_size("sp")
    tok, width = resid.shape
    head = queries_first.shape[1] // rel_first.shape[0]
    kernel, scratch = build_kernel(n, tok, head, width, REACH)
    hbm = pl.BlockSpec(memory_space=pltpu.HBM)
    vmem = pl.BlockSpec(memory_space=pltpu.VMEM)
    return pl.pallas_call(
        kernel,
        out_shape=jax.ShapeDtypeStruct((tok, width), BF16),
        in_specs=[hbm] * 9 + [vmem] * 5,
        out_specs=vmem,
        scratch_shapes=scratch,
        compiler_params=pltpu.CompilerParams(
            collective_id=0, has_side_effects=True, vmem_limit_bytes=60 * 2**20
        ),
    )(
        queries_first, keys_first, values_first, query_weight, key_weight, value_weight, resid,
        out_first, out_second, rel_first, rel_second,
        post_first[None], pre_second[None], post_second[None],
    )


def solution(mesh):
    in_specs = (
        P(("grp", "sp"), None),
        P(("grp", "sp"), "tp"),
        P(("grp", "sp"), "tp"),
        P(("grp", "sp"), "tp"),
        P("tp", None),
        P(),
        P("tp", "sp"),
        P(),
        P("sp", "tp"),
        P("sp", "tp"),
        P("sp", "tp"),
        P("tp", None),
        P(),
        P("tp", "sp"),
    )
    out_specs = P(("grp", "sp"), None)
    return jax.shard_map(shards, mesh=mesh, in_specs=in_specs, out_specs=out_specs, check_vma=False)
```

```python
import jax
import jax.numpy as jnp
from jax import lax
from jax.experimental import pallas as pl
from jax.experimental.pallas import tpu as pltpu
from jax.sharding import PartitionSpec as P

MESH = pl.DeviceIdType.MESH
BF16 = jnp.bfloat16
F32 = jnp.float32

SEG = 64
LEFT = 8
REACH = 512
REL_CLIP = 128


EPS = 1e-06
NEG_FILL = -1e30


def from_behind(value, axis, steps):
    count = lax.axis_size(axis)
    initial, last = (max(0, -steps), min(count, count - steps))
    return lax.ppermute(value, axis, [(source, source + steps) for source in range(initial, last)])


def band_bias(bias_table):
    heads_here = bias_table.shape[0]
    band = (LEFT + 1) * SEG
    length = SEG + band
    index = jnp.arange(length, dtype=jnp.int32)
    distance = jnp.where(index < band, LEFT * SEG - index, LEFT * SEG + length - index)
    slot = jnp.clip(distance, -REL_CLIP, REL_CLIP) + REL_CLIP
    onehot = (slot[:, None] == jnp.arange(2 * REL_CLIP + 1, dtype=jnp.int32)[None, :]).astype(
        jnp.float32
    )
    diagonal_values = jnp.dot(bias_table, onehot.T, precision=lax.Precision.HIGHEST)
    spread = jnp.broadcast_to(diagonal_values[:, None, :], (heads_here, SEG, length)).reshape(
        heads_here, SEG * length
    )
    return spread[:, : SEG * (length - 1)].reshape(heads_here, SEG, length - 1)[:, :, :band]


def attend_band(queries, key_rows, value_rows, bias, key_live):
    rows, width = queries.shape
    heads_here = bias.shape[0]
    head_size = width // heads_here
    blocks = rows // SEG
    query_seg = queries.reshape(blocks, SEG, heads_here, head_size)
    key_seg = key_rows.reshape(blocks + LEFT, SEG, heads_here, head_size)
    value_seg = value_rows.reshape(blocks + LEFT, SEG, heads_here, head_size)
    live_seg = key_live.reshape(blocks + LEFT, SEG)
    key_band = jnp.concatenate(
        [key_seg[earlier : earlier + blocks] for earlier in range(LEFT + 1)], axis=1
    )
    value_band = jnp.concatenate(
        [value_seg[earlier : earlier + blocks] for earlier in range(LEFT + 1)], axis=1
    )
    live_band = jnp.concatenate(
        [live_seg[earlier : earlier + blocks] for earlier in range(LEFT + 1)], axis=1
    )
    scores = jnp.einsum("nqhd,nkhd->nhqk", query_seg, key_band, preferred_element_type=jnp.float32)
    scores = scores * head_size ** (-0.5) + bias[None]
    scores = jnp.where(live_band[:, None, None, :], scores, NEG_FILL)
    largest = jnp.max(scores, axis=-1, keepdims=True)
    weights = jnp.exp(scores - largest)
    weights = (weights / jnp.sum(weights, axis=-1, keepdims=True)).astype(jnp.bfloat16)
    mixed = jnp.einsum("nhqk,nkhd->nqhd", weights, value_band, preferred_element_type=jnp.float32)
    return mixed.astype(jnp.bfloat16).reshape(rows, width)


def extend_rows(pieces, member, own_rows):
    joined = jnp.concatenate([piece[member] for piece in pieces] + [own_rows], axis=0)
    return joined


def normed(hidden, gain):
    values = hidden.astype(jnp.float32)
    scale = lax.rsqrt(jnp.mean(values * values, axis=-1, keepdims=True) + EPS)
    return (values * scale * gain).astype(jnp.bfloat16)


def residual_add(branch, residual, gain):
    values = branch.astype(jnp.float32)
    scale = lax.rsqrt(jnp.mean(values * values, axis=-1, keepdims=True) + EPS)
    return (residual.astype(jnp.float32) + values * scale * gain).astype(jnp.bfloat16)


def combine(mixed, weight, residual, gain):
    partial_rows = jnp.dot(
        mixed, lax.all_gather(weight, "sp", axis=1, tiled=True), preferred_element_type=jnp.float32
    )
    branch = lax.psum_scatter(
        partial_rows.astype(jnp.bfloat16), "tp", scatter_dimension=0, tiled=True
    )
    return residual_add(branch, residual, gain)


def full_rows(share):
    return lax.all_gather(share, "tp", axis=0, tiled=True)


def shards(
    resid,
    queries_first,
    keys_first,
    values_first,
    rel_first,
    post_first,
    out_first,
    pre_second,
    query_weight,
    key_weight,
    value_weight,
    rel_second,
    post_second,
    out_second,
):
    tok_rows = resid.shape[0]
    n_sp = lax.axis_size("sp")
    if (
        rel_first.shape[0] == n_sp
        and n_sp % 2 == 0
        and lax.axis_size("tp") == 2
        and lax.axis_size("grp") == 2
        and REACH % tok_rows == 0
        and tok_rows == REL_CLIP
    ):
        return by_heads(
            resid, queries_first, keys_first, values_first, rel_first, post_first, out_first,
            pre_second, query_weight, key_weight, value_weight, rel_second, post_second, out_second,
        )
    depth = (REACH + tok_rows - 1) // tok_rows
    anchor = lax.axis_index("sp") * tok_rows
    key_live = anchor - REACH + jnp.arange(tok_rows + REACH, dtype=jnp.int32) >= 0
    share_rows = tok_rows // lax.axis_size("tp")
    base_rows = lax.dynamic_slice_in_dim(resid, lax.axis_index("tp") * share_rows, share_rows, 0)
    earlier_first = [
        from_behind((keys_first, values_first), "sp", distance) for distance in range(depth, 0, -1)
    ]
    key_ext = extend_rows(earlier_first, 0, keys_first)
    value_ext = extend_rows(earlier_first, 1, values_first)
    first = attend_band(queries_first, key_ext, value_ext, band_bias(rel_first), key_live)
    hidden_one = combine(first, out_first, base_rows, post_first)
    inputs_two = full_rows(normed(hidden_one, pre_second))
    query_sum = jnp.dot(
        inputs_two,
        lax.all_gather(query_weight, "sp", axis=0, tiled=True),
        preferred_element_type=jnp.float32,
    )
    key_sum = jnp.dot(
        inputs_two,
        lax.all_gather(key_weight, "sp", axis=0, tiled=True),
        preferred_element_type=jnp.float32,
    )
    value_sum = jnp.dot(
        inputs_two,
        lax.all_gather(value_weight, "sp", axis=0, tiled=True),
        preferred_element_type=jnp.float32,
    )
    queries_two = query_sum.astype(jnp.bfloat16)
    keys_two = key_sum.astype(jnp.bfloat16)
    values_two = value_sum.astype(jnp.bfloat16)
    earlier_second = [
        from_behind((keys_two, values_two), "sp", distance) for distance in range(depth, 0, -1)
    ]
    key_ext_two = extend_rows(earlier_second, 0, keys_two)
    value_ext_two = extend_rows(earlier_second, 1, values_two)
    second = attend_band(queries_two, key_ext_two, value_ext_two, band_bias(rel_second), key_live)
    hidden_two = combine(second, out_second, hidden_one, post_second)
    return full_rows(hidden_two)


def scaled(values):
    return values * lax.rsqrt(jnp.mean(values * values, axis=-1, keepdims=True) + EPS)


def build_kernel(n, tok, head, width, reach):
    share = tok // 2
    cols = width // n
    span = reach + tok
    model = width

    def kernel(
        q_hbm, k_hbm, v_hbm, wq_hbm, wk_hbm, wv_hbm, resid_hbm, o1_hbm, o2_hbm,
        rel1, rel2, post1, pre2, post2,
        out_ref,
        heads, weights, outs, res, bias, mixed1, mixed2, parts, inbox, joined, branch, rows2, total, last,
        loc_sem, hs, hr, ws, wr, wf, fs, fr, gs, gr, ps, pr, bs, br, xs, xr, ys, yr,
    ):
        s = lax.axis_index("sp")
        t = lax.axis_index("tp")
        g = lax.axis_index("grp")
        u = 1 - t
        side = s + 1 - 2 * lax.rem(s, 2)

        def rcopy(src, dst, ssem, rsem, sp, tp, grp=g):
            return pltpu.make_async_remote_copy(
                src_ref=src, dst_ref=dst, send_sem=ssem, recv_sem=rsem,
                device_id={"grp": grp, "sp": sp, "tp": tp}, device_id_type=MESH,
            )

        def peer(k):
            return lax.rem(s + k, n)

        barrier = pltpu.get_barrier_semaphore()
        for k in range(n):
            if k:
                pl.semaphore_signal(
                    barrier, inc=1, device_id={"sp": peer(k), "tp": t}, device_id_type=MESH
                )
            pl.semaphore_signal(
                barrier, inc=1, device_id={"sp": peer(k), "tp": u}, device_id_type=MESH
            )
        pl.semaphore_signal(
            barrier, inc=1, device_id={"grp": 1 - g, "sp": s, "tp": t}, device_id_type=MESH
        )
        pl.semaphore_wait(barrier, 2 * n)

        def lanes(j):
            return pl.ds(pl.multiple_of(j * head, head), head)

        def trows(j, base=0):
            return pl.ds(pl.multiple_of(base + j * tok, tok), tok)

        wrows = width // n

        def head_copy(i, ref, j, src):
            dst = heads.at[i, trows(src, reach)]
            return rcopy(ref.at[:, lanes(j)], dst, hs.at[i, j], hr.at[i, src], j, t)

        hrows = wrows // 2

        def weight_half(i, src, part):
            start = pl.multiple_of(src * wrows + part * hrows, hrows)
            return weights.at[pl.ds(start, hrows), pl.ds(i * head, head)]

        def weight_copy(i, j, src):
            piece = wqkv[i].at[pl.ds(pl.multiple_of(g * hrows, hrows), hrows), lanes(j)]
            return rcopy(piece, weight_half(i, src, g), ws.at[i, j], wr.at[i, src, g], j, t)

        def weight_hand(i, src):
            piece = weight_half(i, src, g)
            return rcopy(piece, piece, wf.at[i, src], wr.at[i, src, g], s, t, 1 - g)

        def weight_handed(i, src):
            piece = weight_half(i, src, 1 - g)
            return rcopy(piece, piece, wf.at[i, src], wr.at[i, src, 1 - g], s, t, 1 - g)

        def own_weights(i):
            return pltpu.make_async_copy(
                wqkv[i].at[:, lanes(s)],
                weights.at[pl.ds(pl.multiple_of(s * wrows, wrows), wrows), pl.ds(i * head, head)],
                wr.at[i, s, 0],
            )

        qkv = (q_hbm, k_hbm, v_hbm)
        wqkv = (wq_hbm, wk_hbm, wv_hbm)
        for k in range(1, n):
            for i in range(3):
                head_copy(i, qkv[i], peer(k), s).start()
        for i in range(3):
            pltpu.make_async_copy(
                qkv[i].at[:, lanes(s)], heads.at[i, trows(s, reach)], hr.at[i, s]
            ).start()
        for i in range(3):
            own_weights(i).start()

        def send_weights():
            for i in range(3):
                for k in range(1, n):
                    weight_copy(i, peer(k), s).start()

        local = [
            pltpu.make_async_copy(o1_hbm, outs.at[0], loc_sem.at[0]),
            pltpu.make_async_copy(o2_hbm, outs.at[1], loc_sem.at[1]),
            pltpu.make_async_copy(
                resid_hbm.at[pl.ds(pl.multiple_of(t * share, share), share)], res, loc_sem.at[2]
            ),
        ]
        for copy in local:
            copy.start()

        near = 2 * REL_CLIP
        query = lax.broadcasted_iota(jnp.int32, (tok, span), 0) // SEG
        key = lax.broadcasted_iota(jnp.int32, (tok, span), 1) // SEG
        live = (key >= query) & (key <= query + LEFT)
        for layer, rel in enumerate((rel1, rel2)):
            table = rel[pl.ds(s, 1), :]
            top = table[:, near : near + 1]
            entry = lax.broadcasted_iota(jnp.int32, (near, near + tok), 0)
            place = lax.broadcasted_iota(jnp.int32, (near, near + tok), 1)
            flip = (entry + place == near).astype(F32)
            line = jnp.dot(
                jnp.broadcast_to(table[:, :near], (8, near)), flip,
                preferred_element_type=F32, precision=lax.Precision.HIGHEST,
            )[:1]
            spot = lax.broadcasted_iota(jnp.int32, line.shape, 1)
            line = jnp.where((spot == 0) | (spot >= near), top, line)
            spread = jnp.broadcast_to(line, (tok, near + tok))
            row = lax.broadcasted_iota(jnp.int32, spread.shape, 0)
            step = 1
            while step < tok:
                moved = pltpu.roll(spread, step, 1)
                spread = jnp.where(lax.rem(row // step, 2) == 1, moved, spread)
                step *= 2
            far = jnp.broadcast_to(top, (tok, span - near))
            whole = jnp.concatenate([far, spread[:, :near]], axis=1)
            bias[layer] = jnp.where(live, whole, NEG_FILL)

        heads[1, :reach] = jnp.zeros((reach, head), BF16)
        heads[2, :reach] = jnp.zeros((reach, head), BF16)

        def attend(layer, b):
            q = heads[0, trows(b, reach)]
            k = heads[1, pl.ds(pl.multiple_of(b * tok, tok), span)]
            v = heads[2, pl.ds(pl.multiple_of(b * tok, tok), span)]
            scores = lax.dot_general(
                q, k, (((1,), (1,)), ((), ())), preferred_element_type=F32
            ) * head ** (-0.5) + bias[layer]
            column = lax.broadcasted_iota(jnp.int32, scores.shape, 1)
            scores = jnp.where(column >= reach - b * tok, scores, NEG_FILL)
            e = jnp.exp(scores - jnp.max(scores, axis=-1, keepdims=True))
            e = (e * (1.0 / jnp.sum(e, axis=-1, keepdims=True))).astype(BF16)
            return jnp.dot(e, v, preferred_element_type=F32).astype(BF16)

        def layer_branch(layer, mixed, ms, mr, wait_block, after_own):
            def mcopy(b, src, k, sp):
                block = mixed.at[src, trows(b)]
                return rcopy(block, block, ms.at[b, k], mr.at[b, src], sp, t)

            half = n // 2

            def forward(b):
                for k in range(1, half):
                    mcopy(b, peer(2 * k), k, side).wait_recv()
                    mcopy(b, peer(2 * k), half - 1 + k, side).start()

            def own(b, _):
                wait_block(b)
                mixed[s, trows(b)] = attend(layer, b)
                mcopy(b, s, 0, side).start()
                for k in range(1, half):
                    mcopy(b, s, k, peer(2 * k)).start()

                @pl.when(b >= half)
                def _():
                    forward(b - half)

                return 0

            lax.fori_loop(0, n, own, 0)
            after_own()

            def pcopy(b):
                return rcopy(
                    parts.at[layer, b, u], inbox.at[layer, b],
                    ps.at[layer, b], pr.at[layer, b], s, u,
                )

            def bcopy(b, src):
                return rcopy(
                    joined.at[layer, b], branch.at[layer, src],
                    bs.at[layer, b], br.at[layer, src], b, t,
                )

            def project(b):
                for k in range(half):
                    mcopy(b, lax.rem(side + 2 * k, n), k, side).wait_recv()
                lhs = jnp.concatenate([mixed[j, trows(b)] for j in range(n)], axis=1)
                part = jnp.dot(lhs, outs[layer], preferred_element_type=F32).astype(BF16)
                parts[layer, b, 0] = part[:share]
                parts[layer, b, 1] = part[share:]
                pcopy(b).start()

            def join(b):
                pcopy(b).wait_recv()
                both = parts[layer, b, t].astype(F32) + inbox[layer, b].astype(F32)
                joined[layer, b] = both.astype(BF16)

                @pl.when(b != s)
                def _():
                    bcopy(b, s).start()

                @pl.when(b == s)
                def _():
                    pltpu.make_async_copy(
                        joined.at[layer, b], branch.at[layer, s], br.at[layer, s]
                    ).start()

            def step(b, _):
                @pl.when(b < half)
                def _():
                    forward(n - half + b)

                project(b)

                @pl.when(b > 0)
                def _():
                    join(b - 1)

                return 0

            lax.fori_loop(0, n, step, 0)
            join(n - 1)

            def arrived(j, _):
                bcopy(side, j).wait_recv()
                return 0

            lax.fori_loop(0, n, arrived, 0)

            def drain(b, _):
                for k in range(2 * half - 1):
                    mcopy(b, s, k, side).wait_send()
                pcopy(b).wait_send()

                @pl.when(b != s)
                def _():
                    bcopy(b, s).wait_send()

                return 0

            values = jnp.concatenate([branch[layer, j] for j in range(n)], axis=1)
            return values.astype(F32), drain

        def heads_ready(b):
            for i in range(3):
                head_copy(i, qkv[i], side, b).wait_recv()

        local[0].wait()
        local[1].wait()
        values, drain1 = layer_branch(0, mixed1, fs, fr, heads_ready, send_weights)
        local[2].wait()
        hidden = (res[...].astype(F32) + scaled(values) * post1[...]).astype(BF16)
        res[...] = hidden
        rows2[2 * s + t] = (scaled(hidden.astype(F32)) * pre2[...]).astype(BF16)

        half = n // 2
        wide = width // half

        def xcopy(src, c, k, sp, tp, m):
            block = rows2.at[2 * src + c, :, pl.ds(pl.multiple_of(m * wide, wide), wide)]
            return rcopy(block, block, xs.at[src, k, m], xr.at[2 * src + c, m], sp, tp)

        def xsend(m, _):
            for k in range(1, half):
                xcopy(s, t, k + 1, peer(2 * k), t, m).start()
            xcopy(s, t, 0, side, t, m).start()
            xcopy(s, t, 1, s, u, m).start()
            return 0

        lax.fori_loop(0, half, xsend, 0)

        def hand_weights(k, _):
            for i in range(3):
                weight_copy(i, side, peer(k)).wait_recv()
                weight_hand(i, peer(k)).start()
            return 0

        lax.fori_loop(1, n, hand_weights, 0)

        def near_rows(m, _):
            for k in range(1, half):
                src = peer(2 * k)
                xcopy(src, t, 0, side, t, m).wait_recv()
                xcopy(src, t, 0, side, t, m).start()
                xcopy(src, t, 1, s, u, m).start()
            return 0

        lax.fori_loop(0, half, near_rows, 0)

        def weights_ready(k, _):
            for i in range(3):
                weight_handed(i, peer(k)).wait_recv()
            return 0

        lax.fori_loop(1, n, weights_ready, 0)
        for i in range(3):
            own_weights(i).wait()

        def project_rows(m):
            for src in range(n):
                xcopy(src, u, 1, s, u, m).wait_recv()
            depth = pl.ds(pl.multiple_of(m * wide, wide), wide)
            lhs = rows2[:, :, depth].reshape(n * tok, wide)
            total[...] += jnp.dot(lhs, weights[depth, :], preferred_element_type=F32)

        total[...] = jnp.zeros_like(total)

        def far_rows(m, _):
            for k in range(half):
                src = lax.rem(side + 2 * k, n)
                xcopy(src, t, 0, side, t, m).wait_recv()
                xcopy(src, t, 1, s, u, m).start()

            @pl.when(m > 0)
            def _():
                project_rows(m - 1)

            return 0

        lax.fori_loop(0, half, far_rows, 0)
        project_rows(half - 1)
        for i in range(3):
            heads[i, reach:] = total[:, i * head : (i + 1) * head].astype(BF16)

        values, drain2 = layer_branch(1, mixed2, gs, gr, lambda b: None, lambda: None)
        done = (res[...].astype(F32) + scaled(values) * post2[...]).astype(BF16)
        last[t] = done
        final = rcopy(last.at[t], last.at[t], ys, yr, s, u)
        final.start()

        lax.fori_loop(0, n, lambda b, c: drain1(b, c), 0)
        lax.fori_loop(0, n, lambda b, c: drain2(b, c), 0)
        def drain_first(k, _):
            for i in range(3):
                head_copy(i, qkv[i], peer(k), s).wait_send()
                weight_copy(i, peer(k), s).wait_send()
                weight_hand(i, peer(k)).wait_send()
            return 0

        lax.fori_loop(1, n, drain_first, 0)

        def drain_rows(m, _):
            for k in range(half + 1):
                xcopy(s, t, k, side, t, m).wait_send()
            for k in range(1, half):
                xcopy(peer(2 * k), t, 0, side, t, m).wait_send()
                xcopy(peer(2 * k), t, 1, side, t, m).wait_send()
            for k in range(half):
                xcopy(lax.rem(side + 2 * k, n), t, 1, side, t, m).wait_send()
            return 0

        lax.fori_loop(0, half, drain_rows, 0)
        final.wait_send()
        rcopy(last.at[u], last.at[u], ys, yr, s, u).wait_recv()
        out_ref[:share] = last[0]
        out_ref[share:] = last[1]

    half = n // 2
    scratch = [
        pltpu.VMEM((3, reach + n * tok, head), BF16),
        pltpu.VMEM((width, 3 * head), BF16),
        pltpu.VMEM((2, n * head, cols), BF16),
        pltpu.VMEM((share, width), BF16),
        pltpu.VMEM((2, tok, span), F32),
        pltpu.VMEM((n, n * tok, head), BF16),
        pltpu.VMEM((n, n * tok, head), BF16),
        pltpu.VMEM((2, n, 2, share, cols), BF16),
        pltpu.VMEM((2, n, share, cols), BF16),
        pltpu.VMEM((2, n, share, cols), BF16),
        pltpu.VMEM((2, n, share, cols), BF16),
        pltpu.VMEM((2 * n, share, width), BF16),
        pltpu.VMEM((n * tok, 3 * head), F32),
        pltpu.VMEM((2, share, width), BF16),
        pltpu.SemaphoreType.DMA((3,)),
        pltpu.SemaphoreType.DMA((3, n)),
        pltpu.SemaphoreType.DMA((3, n)),
        pltpu.SemaphoreType.DMA((3, n)),
        pltpu.SemaphoreType.DMA((3, n, 2)),
        pltpu.SemaphoreType.DMA((3, n)),
        pltpu.SemaphoreType.DMA((n, 2 * half - 1)),
        pltpu.SemaphoreType.DMA((n, n)),
        pltpu.SemaphoreType.DMA((n, 2 * half - 1)),
        pltpu.SemaphoreType.DMA((n, n)),
        pltpu.SemaphoreType.DMA((2, n)),
        pltpu.SemaphoreType.DMA((2, n)),
        pltpu.SemaphoreType.DMA((2, n)),
        pltpu.SemaphoreType.DMA((2, n)),
        pltpu.SemaphoreType.DMA((n, half + 1, half)),
        pltpu.SemaphoreType.DMA((2 * n, half)),
        pltpu.SemaphoreType.DMA,
        pltpu.SemaphoreType.DMA,
    ]
    return kernel, scratch


def by_heads(
    resid, queries_first, keys_first, values_first, rel_first, post_first, out_first, pre_second,
    query_weight, key_weight, value_weight, rel_second, post_second, out_second,
):
    n = lax.axis_size("sp")
    tok, width = resid.shape
    head = queries_first.shape[1] // rel_first.shape[0]
    kernel, scratch = build_kernel(n, tok, head, width, REACH)
    hbm = pl.BlockSpec(memory_space=pltpu.HBM)
    vmem = pl.BlockSpec(memory_space=pltpu.VMEM)
    return pl.pallas_call(
        kernel,
        out_shape=jax.ShapeDtypeStruct((tok, width), BF16),
        in_specs=[hbm] * 9 + [vmem] * 5,
        out_specs=vmem,
        scratch_shapes=scratch,
        compiler_params=pltpu.CompilerParams(
            collective_id=0, has_side_effects=True, vmem_limit_bytes=60 * 2**20
        ),
    )(
        queries_first, keys_first, values_first, query_weight, key_weight, value_weight, resid,
        out_first, out_second, rel_first, rel_second,
        post_first[None], pre_second[None], post_second[None],
    )


def solution(mesh):
    in_specs = (
        P(("grp", "sp"), None),
        P(("grp", "sp"), "tp"),
        P(("grp", "sp"), "tp"),
        P(("grp", "sp"), "tp"),
        P("tp", None),
        P(),
        P("tp", "sp"),
        P(),
        P("sp", "tp"),
        P("sp", "tp"),
        P("sp", "tp"),
        P("tp", None),
        P(),
        P("tp", "sp"),
    )
    out_specs = P(("grp", "sp"), None)
    return jax.shard_map(shards, mesh=mesh, in_specs=in_specs, out_specs=out_specs, check_vma=False)
```
